32 devices in a mesh: ep: 8 (over z, core), tp: 4 (over y, x).
Axes of the slice: x: 2, y: 2, z: 4, core: 2. Of those that a mesh axis runs over, the one named last changes fastest.
Arguments:
- tokens: bfloat16 [1024, 4096], P('ep', 'tp'), may hold values from -6 to 6
- routes: int32 [1024, 2], P('ep'), may hold values from 0 to 15, all different within a row; in each aligned block of 128 rows (0 to 127, 128 to 255, ...) at most 20 rows name the same one
- route_weights: float32 [1024, 2], P('ep'), may hold values from 0.2 to 2
- cotangent: bfloat16 [1024, 4096], P('ep', 'tp'), may hold values from -6 to 6
- expert_gate: bfloat16 [16, 4096, 512], P('ep', 'tp'), may hold values from -0.09375 to 0.09375
- expert_up: bfloat16 [16, 4096, 512], P('ep', 'tp'), may hold values from -0.09375 to 0.09375
- expert_down: bfloat16 [16, 512, 4096], P('ep', None, 'tp'), may hold values from -0.25 to 0.25
- shared_gate: bfloat16 [4096, 512], P('tp'), may hold values from -0.09375 to 0.09375
- shared_up: bfloat16 [4096, 512], P('tp'), may hold values from -0.09375 to 0.09375
- shared_down: bfloat16 [512, 4096], P(None, 'tp'), may hold values from -0.25 to 0.25
Outputs:
- grad_tokens: bfloat16 [1024, 4096], P('ep', 'tp')
- grad_weights: float32 [1024, 2], P('ep')
- grad_expert_gate: float32 [16, 4096, 512], P('ep', 'tp')
- grad_expert_up: float32 [16, 4096, 512], P('ep', 'tp')
- grad_expert_down: float32 [16, 512, 4096], P('ep', None, 'tp')
- grad_shared_gate: float32 [4096, 512], P('tp', 'ep')
- grad_shared_up: float32 [4096, 512], P('tp', 'ep')
- grad_shared_down: float32 [512, 4096], P('ep', 'tp')
The draws below stay inside these ranges and needn't reach their ends.
Inputs may be any that keep to these rules, and one draw needn't show every extreme that they name: `routes`: each row names 2 different experts. In each aligned block of 128 rows (the rows of one index of ep) no expert is named by more than 20 rows, a bound that some block reaches.
All inputs are finite; a program needn't handle non-finite values.
Results may differ from the reference program's by a relative error of at most 0.0054.
Values may be sent and summed in bfloat16 or wider, within the bound.
A program may use at most 64 MiB of HBM per device.

```python
import math
import jax
import jax.numpy as jnp
import numpy as np
from jax import lax

D = 4096
FF = 512
SFF = 512
TOPK = 2
TOK_DEV = 128
EXPERTS = 16
CAP = 20
TOKENS = 1024
N_EP = 8


def levels(own_key, shape, cuts, least, largest):
    def one(position, parts):
        heights = jax.random.uniform(jax.random.fold_in(jax.random.fold_in(own_key, 6), position), (parts,), jnp.float32, least / len(cuts), largest / len(cuts))
        return jnp.repeat(jnp.exp(heights), shape[position] // parts).reshape((-1,) + (1,) * (len(shape) - position - 1))

    level = one(*cuts[0])
    for cut in cuts[1:]:
        level = level * one(*cut)
    return level


def routed_block(own_key, own, number, rows, count, top, reach, lean):
    ranking = jax.random.permutation(own_key, count)
    heavy_load, common = portions_of(count, rows * top, reach, lean, True), portions_of(count, rows * top, reach, lean, False)
    places = jnp.arange(count)

    def named(lengths, rotation):
        used = int((lengths > 0).sum())
        fixed = max(1, used // 4)
        shifted = fixed + (places - fixed + rotation * (used - fixed)) % max(1, count - fixed)
        return jnp.zeros((count,), jnp.int32).at[ranking[jnp.where(places < fixed, places, shifted)]].set(jnp.asarray(lengths, jnp.int32))

    lengths = jnp.where(number % 4 == 0, named(heavy_load, number // 4), named(common, number - number // 4 - 1))
    mixed = jax.random.permutation(jax.random.fold_in(own, 3), count)
    giver, sink = mixed[0:count // 2 * 2:2], mixed[1:count // 2 * 2:2]
    margin = jnp.minimum(lengths[giver] - 1, reach - lengths[sink]) // 2
    margin = jnp.where((giver == ranking[0]) | (sink == ranking[0]) | (lengths[sink] == 0), 0, jnp.maximum(margin, 0))
    shifted = jax.random.randint(jax.random.fold_in(own, 4), (count // 2,), 0, 1 << 20) % (margin + 1)
    lengths = lengths.at[giver].add(-shifted).at[sink].add(shifted)
    members = jnp.searchsorted(jnp.cumsum(lengths), jnp.arange(rows * top), side="right").astype(jnp.int32)
    table = members.reshape(top, rows).T
    table = table[jax.random.permutation(jax.random.fold_in(own, 1), rows)]
    rotation = jax.random.randint(jax.random.fold_in(own, 2), (rows, 1), 0, top)
    return jnp.take_along_axis(table, (jnp.arange(top)[None, :] + rotation) % top, axis=1)


def portions_of(number_of, total, most, lean, full):
    loads = [(1 << 20) // math.isqrt(grade ** lean) + 1 for grade in range(1, number_of + 1)]
    largest = most if full else min(most, max(-(-total // number_of), total * loads[0] // sum(loads)))
    least = 1 if total - largest >= number_of - 1 else 0
    given, rest = [largest] + [least] * (number_of - 1), total - largest - least * (number_of - 1)
    while rest > 0:
        free = [i for i in range(1, number_of) if given[i] < largest] or [i for i in range(1, number_of) if given[i] < most]
        pool, remaining = sum([loads[i] for i in free]), rest
        for i in free:
            extra = min(most - given[i], max(1, remaining * loads[i] // pool), rest)
            given[i] = given[i] + extra
            rest = rest - extra
    return np.array(given)


def centred(own_key, dims, width, bound, shards=(), kind=jnp.bfloat16):
    entries = width * jax.random.normal(own_key, dims, jnp.float32)
    if shards:
        entries = entries * levels(own_key, dims, shards, -0.22, 0.18)
    return jnp.clip(entries, -bound, bound).astype(kind)


def setup_inputs(seed: int = 0) -> dict:
    streams_of = jax.random.split(jax.random.key(seed), 11)
    tokens = centred(streams_of[0], (TOKENS, D), 1.0, 6.0, ((0, 8), (1, 4)))
    routes_keys = jax.random.split(jax.random.fold_in(streams_of[1], 1), TOKENS // TOK_DEV)
    routes_turns = jax.random.permutation(jax.random.fold_in(streams_of[1], 3), TOKENS // TOK_DEV)
    routes = jax.vmap(lambda own, number: routed_block(jax.random.fold_in(streams_of[1], 2), own, number, TOK_DEV, EXPERTS, TOPK, CAP, 2))(routes_keys, routes_turns).reshape((TOKENS, TOPK))
    route_weights = jnp.clip(0.2 + 1.8 * jax.random.uniform(streams_of[2], (TOKENS, TOPK), jnp.float32) ** levels(streams_of[2], (TOKENS, TOPK), ((0, 8),), -0.2, 0.2), 0.2, 2.0)
    cotangent = centred(streams_of[3], (TOKENS, D), 1.0, 6.0, ((0, 8), (1, 4)))
    expert_gate = centred(streams_of[4], (EXPERTS, D, FF), D ** -0.5, 0.09375, ((0, 8), (1, 4)))
    expert_up = centred(streams_of[5], (EXPERTS, D, FF), D ** -0.5, 0.09375, ((0, 8), (1, 4)))
    expert_down = centred(streams_of[6], (EXPERTS, FF, D), FF ** -0.5, 0.25, ((0, 8), (2, 4)))
    shared_gate = centred(streams_of[7], (D, SFF), D ** -0.5, 0.09375, ((0, 4),))
    shared_up = centred(streams_of[8], (D, SFF), D ** -0.5, 0.09375, ((0, 4),))
    shared_down = centred(streams_of[9], (SFF, D), SFF ** -0.5, 0.25, ((1, 4),))
    return dict(tokens=tokens, routes=routes, route_weights=route_weights, cotangent=cotangent, expert_gate=expert_gate, expert_up=expert_up, expert_down=expert_down, shared_gate=shared_gate, shared_up=shared_up, shared_down=shared_down)


def rounded(values):
    return lax.optimization_barrier(values.astype(jnp.bfloat16)).astype(jnp.float32)


def hidden_terms(gate_pre, up_pre, back_grad, scaling):
    logistic = jax.nn.sigmoid(gate_pre)
    product = gate_pre * logistic * up_pre
    grad_act = scaling * back_grad
    gate_grad = (grad_act * up_pre * logistic * (1.0 + gate_pre * (1.0 - logistic))).astype(jnp.bfloat16)
    up_grad = (grad_act * gate_pre * logistic).astype(jnp.bfloat16)
    hidden = (scaling * product).astype(jnp.bfloat16)
    return gate_grad, up_grad, hidden, jnp.sum(back_grad * product, axis=-1)


def reference(tokens, routes, route_weights, cotangent, expert_gate, expert_up, expert_down,
              shared_gate, shared_up, shared_down):
    picked = routes.reshape(N_EP, TOK_DEV * TOPK)
    onehot = (picked[:, :, None] == jnp.arange(EXPERTS, dtype=jnp.int32)[None, None, :]).astype(jnp.int32)
    ranked = jnp.sum(jnp.cumsum(onehot, axis=1) * onehot, axis=2) - 1
    block_ids = jnp.arange(N_EP, dtype=jnp.int32)[:, None]
    slot_ids = (picked * (N_EP * CAP) + block_ids * CAP + ranked).reshape(-1).astype(jnp.int32)
    source_ids = jnp.full((EXPERTS * N_EP * CAP,), TOKENS * TOPK, jnp.int32)
    source_ids = source_ids.at[slot_ids].set(jnp.arange(TOKENS * TOPK, dtype=jnp.int32))
    token_ids = (source_ids // TOPK).astype(jnp.int32)
    tokens_pad = jnp.concatenate([tokens, jnp.zeros((1, D), jnp.bfloat16)], axis=0)
    cot_pad = jnp.concatenate([cotangent, jnp.zeros((1, D), jnp.bfloat16)], axis=0)
    gates_pad = jnp.concatenate([rounded(route_weights).reshape(-1), jnp.zeros((1,), jnp.float32)], axis=0)

    def expert_pass(inputs):
        token_index, source_index, weight_gate, weight_up, weight_down = inputs
        slot_tokens = tokens_pad[token_index]
        slot_cotan = cot_pad[token_index]
        slot_gates = gates_pad[source_index]
        gate_pre = jnp.dot(slot_tokens, weight_gate, preferred_element_type=jnp.float32)
        up_pre = jnp.dot(slot_tokens, weight_up, preferred_element_type=jnp.float32)
        back_grad = jnp.dot(slot_cotan, weight_down.T, preferred_element_type=jnp.float32)
        gate_grad, up_grad, hidden, slot_dg = hidden_terms(gate_pre, up_pre, back_grad, slot_gates[:, None])
        slot_grad = (jnp.dot(gate_grad, weight_gate.T, preferred_element_type=jnp.float32)
                     + jnp.dot(up_grad, weight_up.T, preferred_element_type=jnp.float32))
        grad_gate = jnp.dot(slot_tokens.T, gate_grad, preferred_element_type=jnp.float32)
        grad_up = jnp.dot(slot_tokens.T, up_grad, preferred_element_type=jnp.float32)
        grad_down = jnp.dot(hidden.T, slot_cotan, preferred_element_type=jnp.float32)
        return slot_grad, slot_dg, grad_gate, grad_up, grad_down

    slot_grad, slot_dg, grad_expert_gate, grad_expert_up, grad_expert_down = lax.map(
        expert_pass,
        (token_ids.reshape(EXPERTS, N_EP * CAP), source_ids.reshape(EXPERTS, N_EP * CAP),
         expert_gate, expert_up, expert_down))
    routed_grad = slot_grad.reshape(-1, D)[slot_ids].reshape(TOKENS, TOPK, D)
    routed_grad = jnp.sum(routed_grad, axis=1)
    grad_weights = slot_dg.reshape(-1)[slot_ids].reshape(TOKENS, TOPK)

    shared_gate_pre = jnp.dot(tokens, shared_gate, preferred_element_type=jnp.float32)
    shared_up_pre = jnp.dot(tokens, shared_up, preferred_element_type=jnp.float32)
    shared_back = jnp.dot(cotangent, shared_down.T, preferred_element_type=jnp.float32)
    shared_gate_grad, shared_up_grad, shared_hidden, unused_sum = hidden_terms(
        shared_gate_pre, shared_up_pre, shared_back, 1.0)
    shared_grad = (jnp.dot(shared_gate_grad, shared_gate.T, preferred_element_type=jnp.float32)
                   + jnp.dot(shared_up_grad, shared_up.T, preferred_element_type=jnp.float32))
    grad_shared_gate = jnp.dot(tokens.T, shared_gate_grad, preferred_element_type=jnp.float32)
    grad_shared_up = jnp.dot(tokens.T, shared_up_grad, preferred_element_type=jnp.float32)
    grad_shared_down = jnp.dot(shared_hidden.T, cotangent, preferred_element_type=jnp.float32)
    grad_tokens = (routed_grad + shared_grad).astype(jnp.bfloat16)
    return (grad_tokens, grad_weights, grad_expert_gate, grad_expert_up, grad_expert_down,
            grad_shared_gate, grad_shared_up, grad_shared_down)
```

```python
import functools

import jax
import jax.numpy as jnp
from jax import lax
from jax.experimental import pallas as pl
from jax.experimental.pallas import tpu as pltpu
from jax.sharding import PartitionSpec as P

CORES = 2
BF = jnp.bfloat16
F32 = jnp.float32


def up_to(value, unit):
    return -(-value // unit) * unit


def dot(a, b):
    return jnp.dot(a, b, preferred_element_type=F32)


def dot_t(a, b):
    return lax.dot_general(a, b, (((1,), (1,)), ((), ())), preferred_element_type=F32)


def hidden_terms(gate_pre, up_pre, back_grad, scaling):
    logistic = jax.nn.sigmoid(gate_pre)
    silu = gate_pre * logistic
    product = silu * up_pre
    grad_act = back_grad if scaling is None else scaling * back_grad
    gate_grad = grad_act * up_pre * logistic * (1.0 + gate_pre * (1.0 - logistic))
    hidden = product if scaling is None else scaling * product
    return (
        gate_grad.astype(BF),
        (grad_act * silu).astype(BF),
        hidden.astype(BF),
        jnp.sum(back_grad * product, axis=-1, keepdims=True),
    )


def ring_plan(length):
    plan = []
    for step in range(1, length // 2 + 1):
        last_even = length % 2 == 0 and step == length // 2
        plan.append((step, 0, (0,) if last_even else (0, 1)))
        plan.append((step, 1, (1,) if last_even else (1, 0)))
    return plan


def kernel(
    dims,
    meta_in,
    home_in,
    tok_in,
    cot_in,
    eg_in,
    eu_in,
    ed_in,
    sg_in,
    su_in,
    sd_in,
    gtok_out,
    gw_out,
    osg,
    osu,
    osd,
    stok,
    scot,
    hg,
    hu,
    hh,
    all_tok,
    all_cot,
    all_meta,
    eg,
    eu,
    ed,
    sg,
    su,
    sd,
    sel,
    gates,
    sh_part,
    sh_recv,
    sh_all,
    share_t,
    part,
    recv,
    dgs,
    sgrad,
    back_send,
    back,
    shsum,
    load_sem,
    own_sem,
    ring_s,
    ring_r,
    mate_s,
    mate_r,
    shr_s,
    shr_r,
    sha_s,
    sha_r,
    pr_s,
    pr_r,
    pa_s,
    pa_r,
    xt_s,
    xt_r,
    bk_s,
    bk_r,
):
    ep, tp, tok, dl, ne, ff, sff, cap, re, rows, rpp, rpt, hp, swid = dims
    me = lax.axis_index("ep")
    mt = lax.axis_index("tp")
    length = ep // CORES
    chip = me // CORES
    core = me % CORES
    mate = chip * CORES + (1 - core)
    nxt = ((chip + 1) % length) * CORES + core
    prv = ((chip + length - 1) % length) * CORES + core

    owns = []
    for n, (src, dst) in enumerate(((tok_in, all_tok), (cot_in, all_cot), (meta_in, all_meta))):
        c = pltpu.make_async_copy(src, dst.at[me], own_sem.at[n])
        c.start()
        owns.append(c)
    loads = []
    for n, (src, dst) in enumerate(
        ((sg_in, sg), (su_in, su), (sd_in, sd), (eg_in, eg), (eu_in, eu), (ed_in, ed))
    ):
        c = pltpu.make_async_copy(src, dst, load_sem.at[n])
        c.start()
        loads.append(c)

    barrier = pltpu.get_barrier_semaphore()
    for o in range(1, ep):
        pl.semaphore_signal(barrier, inc=1, device_id={"ep": (me + o) % ep})
    for o in range(1, tp):
        pl.semaphore_signal(barrier, inc=1, device_id={"tp": (mt + o) % tp})
    pl.semaphore_wait(barrier, ep + tp - 2)

    sends = []

    def remote(src, dst, ssem, rsem, dev):
        c = pltpu.make_async_remote_copy(
            src_ref=src, dst_ref=dst, send_sem=ssem, recv_sem=rsem, device_id=dev
        )
        c.start()
        sends.append(c)
        return c

    bufs = (all_tok, all_cot, all_meta)
    ring_copies = {}
    mate_copies = []
    plan = {(step, d): items for step, d, items in ring_plan(length)}

    def ring_send(step, d, item, src):
        dest = nxt if d == 0 else prv
        subs = (0, 2) if item == 0 else (1,)
        for b in subs:
            n = ((step - 1) * 2 + d) * 3 + b
            ring_copies[step, d, b] = remote(
                bufs[b].at[src], bufs[b].at[src], ring_s.at[n], ring_r.at[n], {"ep": dest}
            )

    def mate_send(item, src):
        for b in (0, 2) if item == 0 else (1,):
            n = len(mate_copies)
            mate_copies.append(
                remote(
                    bufs[b].at[src], bufs[b].at[src], mate_s.at[n], mate_r.at[n], {"ep": mate}
                )
            )

    for c in owns:
        c.wait()
    for pos in range(2):
        for d in range(2):
            items = plan.get((1, d), ())
            if pos < len(items):
                ring_send(1, d, items[pos], me)
    mate_send(0, me)
    mate_send(1, me)

    tp_order = [(mt + o) % tp for o in range(1, tp)]
    if rpt * tp > tok:
        sh_part[:, tok:, :] = jnp.zeros((3, rpt * tp - tok, sff), BF)
    for n in range(3):
        loads[n].wait()
        if n < 2:
            val = dot(all_tok[me], (sg, su)[n][...])
        else:
            val = dot_t(all_cot[me], sd[...])
        sh_part[n, :tok, :] = val.astype(BF)
    sh_copies = []
    for o in range(1, tp):
        peer = tp_order[o - 1]
        sh_copies.append(
            remote(
                sh_part.at[:, pl.ds(pl.multiple_of(peer * rpt, 16), rpt), :],
                sh_recv.at[o],
                shr_s.at[o],
                shr_r.at[o],
                {"tp": peer},
            )
        )

    def ring_arrivals(step):
        for pos in range(2):
            for d in range(2):
                items = plan.get((step, d), ())
                if pos >= len(items):
                    continue
                item = items[pos]
                away = length - step if d == 0 else step
                src = ((chip + away) % length) * CORES + core
                for b in (0, 2) if item == 0 else (1,):
                    ring_copies[step, d, b].wait_recv()
                if item in plan.get((step + 1, d), ()):
                    ring_send(step + 1, d, item, src)
                mate_send(item, src)

    if length > 1:
        ring_arrivals(1)

    for c in sh_copies:
        c.wait_recv()
    mine_t = pl.ds(pl.multiple_of(mt * rpt, 16), rpt)
    tot = [sh_part[n, mine_t, :].astype(F32) for n in range(3)]
    for o in range(1, tp):
        for n in range(3):
            tot[n] = tot[n] + sh_recv[o, n].astype(F32)
    a, b, c3, _ = hidden_terms(tot[0], tot[1], tot[2], None)
    sh_all[0, mine_t, :] = a
    sh_all[1, mine_t, :] = b
    sh_all[2, mine_t, :] = c3
    sha = []
    for o in range(1, tp):
        sha.append(
            remote(
                sh_all.at[:, mine_t, :],
                sh_all.at[:, mine_t, :],
                sha_s.at[o],
                sha_r.at[o],
                {"tp": tp_order[o - 1]},
            )
        )

    for step in range(2, length // 2 + 1):
        ring_arrivals(step)
    for c in mate_copies:
        c.wait_recv()

    row_id = lax.broadcasted_iota(jnp.int32, (rows, tok), 0)
    gate = jnp.zeros((rows, 1), F32)
    for j in range(ep):
        m = all_meta[j]
        code = m[0:2, :].astype(jnp.int32) + (j * cap - me * (ne * re))
        p0 = (row_id == code[0:1, :]).astype(F32)
        p1 = (row_id == code[1:2, :]).astype(F32)
        sel[:, j * tok : (j + 1) * tok] = (p0 + p1).astype(BF)
        gate = gate + jnp.sum(p0 * m[2:3, :] + p1 * m[3:4, :], axis=1, keepdims=True)
    gates[:rows, :] = jnp.broadcast_to(gate, (rows, 128))
    total_rows = rpp * tp
    if total_rows > rows:
        gates[rows:, :] = jnp.zeros((total_rows - rows, 128), F32)
        part[:, rows:, :] = jnp.zeros((3, total_rows - rows, ff), BF)

    p_copies = []

    def push(n):
        for o in range(1, tp):
            peer = tp_order[o - 1]
            p_copies.append(
                remote(
                    part.at[n, pl.ds(pl.multiple_of(peer * rpp, 16), rpp), :],
                    recv.at[o, n],
                    pr_s.at[n * tp + o],
                    pr_r.at[n * tp + o],
                    {"tp": peer},
                )
            )

    stok[...] = dot(sel[...], all_tok[...].reshape(ep * tok, dl)).astype(BF)
    for n in range(2):
        loads[3 + n].wait()
        for e in range(ne):
            part[n, e * re : (e + 1) * re, :] = dot(
                stok[e * re : (e + 1) * re, :], (eg, eu)[n][e]
            ).astype(BF)
        push(n)
    scot[...] = dot(sel[...], all_cot[...].reshape(ep * tok, dl)).astype(BF)
    loads[5].wait()
    for e in range(ne):
        part[2, e * re : (e + 1) * re, :] = dot_t(scot[e * re : (e + 1) * re, :], ed[e]).astype(BF)
    push(2)

    for c in sha:
        c.wait_recv()
    for n in range(3):
        back_t = sh_all[n, :tok, :].astype(F32).T.astype(BF)
        for j in range(ep):
            share_t[0, n, j] = back_t[j * swid : (j + 1) * swid, :]
    xts = []
    for o in range(1, ep):
        peer = (me + o) % ep
        xts.append(
            remote(
                share_t.at[0, :, peer],
                share_t.at[1, :, me],
                xt_s.at[o],
                xt_r.at[o],
                {"ep": peer},
            )
        )
    for n in range(3):
        share_t[1, n, me] = share_t[0, n, me]
    shsum[...] = dot_t(sh_all[0, :tok, :], sg[...]) + dot_t(sh_all[1, :tok, :], su[...])

    for c in p_copies:
        c.wait_recv()
    mine = pl.ds(pl.multiple_of(mt * rpp, 16), rpp)
    tot = [part[n, mine, :].astype(F32) for n in range(3)]
    for o in range(1, tp):
        for n in range(3):
            tot[n] = tot[n] + recv[o, n].astype(F32)
    a, b, c3, dg = hidden_terms(tot[0], tot[1], tot[2], gates[mine, :][:, 0:1])
    hg[mine, :] = a
    hu[mine, :] = b
    hh[mine, :] = c3
    high = dg.astype(BF).astype(F32)
    lane = lax.broadcasted_iota(jnp.int32, (rpp, 128), 1)
    dgs[mine, :] = jnp.where(lane == 0, high, jnp.where(lane == 1, dg - high, 0.0)).astype(BF)
    pas = []
    for k, buf in enumerate((hg, hu, dgs, hh)):
        for o in range(1, tp):
            pas.append(
                remote(
                    buf.at[mine, :],
                    buf.at[mine, :],
                    pa_s.at[k * tp + o],
                    pa_r.at[k * tp + o],
                    {"tp": tp_order[o - 1]},
                )
            )

    for c in xts:
        c.wait_recv()
    flat = [
        jnp.concatenate([share_t[1, n, j] for j in range(ep)], axis=1) for n in range(3)
    ]
    tok_flat = all_tok[...].reshape(ep * tok, dl)
    osg[...] = dot(flat[0], tok_flat).T
    osu[...] = dot(flat[1], tok_flat).T
    osd[...] = dot(flat[2], all_cot[...].reshape(ep * tok, dl))

    for c in pas[: 3 * (tp - 1)]:
        c.wait_recv()
    for e in range(ne):
        r = slice(e * re, (e + 1) * re)
        sgrad[r, :dl] = (dot_t(hg[r, :], eg[e]) + dot_t(hu[r, :], eu[e])).astype(BF)
    sgrad[:, dl:] = dgs[:rows, :]
    col = lax.broadcasted_iota(jnp.int32, (8, rows), 1)
    expert = jnp.zeros((8, rows), jnp.int32)
    for e in range(1, ne):
        expert = expert + (col >= e * re).astype(jnp.int32)
    within = col - expert * re
    block = jnp.zeros((8, rows), jnp.int32)
    for j in range(1, ep):
        block = block + (within >= j * cap).astype(jnp.int32)
    target = block * hp + expert * cap + (within - block * cap)
    target = jnp.where(within < ep * cap, target, -1)
    pick = (
        (lax.broadcasted_iota(jnp.int32, (ep * hp, rows), 0) == target[0:1, :])
        .astype(F32)
        .astype(BF)
    )
    back_send[...] = dot(pick, sgrad[...]).astype(BF).reshape(ep, hp, dl + 128)
    bks = []
    for o in range(1, ep):
        peer = (me + o) % ep
        bks.append(
            remote(back_send.at[peer], back.at[me], bk_s.at[o], bk_r.at[o], {"ep": peer})
        )
    back[me] = back_send[me]
    home = home_in[...]
    hcol = lax.broadcasted_iota(jnp.int32, (tok, ep * hp), 1)
    g0 = (hcol == home[:, 0:1]).astype(F32)
    g1 = (hcol == home[:, 1:2]).astype(F32)
    both = (g0 + g1).astype(BF)
    for c in bks:
        c.wait_recv()
    flat_back = back[...].reshape(ep * hp, dl + 128)
    gtok_out[...] = (dot(both, flat_back[:, :dl]) + shsum[...]).astype(BF)
    w0 = jnp.sum(dot(g0.astype(BF), flat_back[:, dl:]), axis=1, keepdims=True)
    w1 = jnp.sum(dot(g1.astype(BF), flat_back[:, dl:]), axis=1, keepdims=True)
    wl = lax.broadcasted_iota(jnp.int32, (tok, 128), 1)
    gw_out[...] = jnp.where(wl == 0, w0, w1)
    for c in pas[3 * (tp - 1) :]:
        c.wait_recv()
    for c in sends:
        c.wait_send()


def body(
    tokens,
    routes,
    route_weights,
    cotangent,
    expert_gate,
    expert_up,
    expert_down,
    shared_gate,
    shared_up,
    shared_down,
):
    tok, top = routes.shape
    dl = tokens.shape[1]
    ne, _, ff = expert_gate.shape
    sff = shared_gate.shape[1]
    ep, tp = lax.axis_size("ep"), lax.axis_size("tp")
    cap = max(2, 5 * tok * top // (4 * ep * ne))
    re = up_to(ep * cap, 16)
    rows = ne * re
    rpp = up_to(-(-rows // tp), 16)
    rpt = up_to(-(-tok // tp), 16)
    hp = up_to(ne * cap, 16)
    swid = sff // ep
    length = ep // CORES
    total = rpp * tp
    dims = (ep, tp, tok, dl, ne, ff, sff, cap, re, rows, rpp, rpt, hp, swid)

    picked = routes.T.reshape(-1)
    earlier = jnp.arange(top * tok)[None, :] < jnp.arange(top * tok)[:, None]
    same = picked[:, None] == picked[None, :]
    ranked = jnp.sum((same & earlier).astype(jnp.int32), axis=1)
    code = (picked * re + ranked).reshape(top, tok)
    home = ((picked // ne) * hp + (picked % ne) * cap + ranked).reshape(top, tok)
    gate = route_weights.astype(BF).astype(F32).T
    meta = jnp.concatenate(
        [code.astype(F32), gate, jnp.zeros((8 - 2 * top, tok), F32)], axis=0
    )

    vm = pl.BlockSpec(memory_space=pltpu.VMEM)
    hbm = pl.BlockSpec(memory_space=pl.ANY)
    dma = pltpu.SemaphoreType.DMA
    n_ring = max(1, (length // 2) * 6)
    scratch = [
        pltpu.VMEM((ep, tok, dl), BF),
        pltpu.VMEM((ep, tok, dl), BF),
        pltpu.VMEM((ep, 8, tok), F32),
        pltpu.VMEM(expert_gate.shape, BF),
        pltpu.VMEM(expert_up.shape, BF),
        pltpu.VMEM(expert_down.shape, BF),
        pltpu.VMEM(shared_gate.shape, BF),
        pltpu.VMEM(shared_up.shape, BF),
        pltpu.VMEM(shared_down.shape, BF),
        pltpu.VMEM((rows, ep * tok), BF),
        pltpu.VMEM((total, 128), F32),
        pltpu.VMEM((3, rpt * tp, sff), BF),
        pltpu.VMEM((tp, 3, rpt, sff), BF),
        pltpu.VMEM((3, rpt * tp, sff), BF),
        pltpu.VMEM((2, 3, ep, swid, tok), BF),
        pltpu.VMEM((3, total, ff), BF),
        pltpu.VMEM((tp, 3, rpp, ff), BF),
        pltpu.VMEM((total, 128), BF),
        pltpu.VMEM((rows, dl + 128), BF),
        pltpu.VMEM((ep, hp, dl + 128), BF),
        pltpu.VMEM((ep, hp, dl + 128), BF),
        pltpu.VMEM((tok, dl), F32),
        dma((6,)),
        dma((3,)),
        dma((n_ring,)),
        dma((n_ring,)),
        dma((3 * length,)),
        dma((3 * length,)),
        dma((tp,)),
        dma((tp,)),
        dma((tp,)),
        dma((tp,)),
        dma((3 * tp,)),
        dma((3 * tp,)),
        dma((4 * tp,)),
        dma((4 * tp,)),
        dma((ep,)),
        dma((ep,)),
        dma((ep,)),
        dma((ep,)),
    ]
    sds = jax.ShapeDtypeStruct
    outs = pl.pallas_call(
        functools.partial(kernel, dims),
        out_shape=(
            sds((tok, dl), BF),
            sds((tok, 128), F32),
            sds((dl, swid), F32),
            sds((dl, swid), F32),
            sds((swid, dl), F32),
            sds((rows, dl), BF),
            sds((rows, dl), BF),
            sds((total, ff), BF),
            sds((total, ff), BF),
            sds((total, ff), BF),
        ),
        in_specs=[hbm, vm] + [hbm] * 8,
        out_specs=tuple([vm] * 10),
        scratch_shapes=scratch,
        compiler_params=pltpu.CompilerParams(
            collective_id=0, has_side_effects=True, vmem_limit_bytes=60 * 1024 * 1024
        ),
    )(
        meta,
        home.T,
        tokens,
        cotangent,
        expert_gate,
        expert_up,
        expert_down,
        shared_gate,
        shared_up,
        shared_down,
    )
    gtok, gw, osg, osu, osd, stok, scot, hg, hu, hh = outs
    stok = stok.reshape(ne, re, dl)
    scot = scot.reshape(ne, re, dl)
    hg, hu, hh = (h[:rows].reshape(ne, re, ff) for h in (hg, hu, hh))
    grad_gate = jnp.einsum("esd,esf->edf", stok, hg, preferred_element_type=F32)
    grad_up = jnp.einsum("esd,esf->edf", stok, hu, preferred_element_type=F32)
    grad_down = jnp.einsum("esf,esd->efd", hh, scot, preferred_element_type=F32)
    return gtok, gw[:, :top], grad_gate, grad_up, grad_down, osg, osu, osd


def solution(mesh):
    return jax.shard_map(
        body,
        mesh=mesh,
        in_specs=(
            P("ep", "tp"),
            P("ep", None),
            P("ep", None),
            P("ep", "tp"),
            P("ep", "tp", None),
            P("ep", "tp", None),
            P("ep", None, "tp"),
            P("tp", None),
            P("tp", None),
            P(None, "tp"),
        ),
        out_specs=(
            P("ep", "tp"),
            P("ep", None),
            P("ep", "tp", None),
            P("ep", "tp", None),
            P("ep", None, "tp"),
            P("tp", "ep"),
            P("tp", "ep"),
            P("ep", "tp"),
        ),
        check_vma=False,
    )
```
